128 devices in a mesh: ep: 32 (over z, y, core), tp: 4 (over x).
Axes of the slice: x: 4, y: 4, z: 4, core: 2. Of those that a mesh axis runs over, the one named last changes fastest.
Arguments:
- queries: bfloat16 [16384, 1024], P('ep', 'tp'), may hold values from -8 to 8
- key_rows: bfloat16 [16384, 1024], P('ep', 'tp'), may hold values from -8 to 8
- value_rows: bfloat16 [16384, 1024], P('ep', 'tp'), may hold values from -6 to 6
- lambdas: float32 [8], P('tp'), may hold values from 0.3 to 0.8
- head_gain: float32 [128], replicated, may hold values from 0.1 to 1.9
- out_weight: bfloat16 [1024, 2048], P('tp'), may hold values from -0.1875 to 0.1875
- moe_input: bfloat16 [16384, 2048], P(('ep', 'tp')), may hold values from -400 to 400
- moe_gain: float32 [2048], replicated, may hold values from 0.1 to 1.9
- routes: int32 [16384, 2], P(('ep', 'tp')), may hold values from 0 to 31, all different within a row; in each aligned block of 128 rows (0 to 127, 128 to 255, ...) at most 10 rows name the same one
- route_logits: float32 [16384, 2], P(('ep', 'tp')), may hold values from -6 to 6
- expert_gate: bfloat16 [32, 2048, 3584], P('ep', None, 'tp'), may hold values from -0.125 to 0.125
- expert_up: bfloat16 [32, 2048, 3584], P('ep', None, 'tp'), may hold values from -0.125 to 0.125
- expert_down: bfloat16 [32, 3584, 2048], P('ep', 'tp'), may hold values from -0.09375 to 0.09375
Outputs:
- mixer_out: bfloat16 [16384, 2048], P(('ep', 'tp'))
- expert_out: bfloat16 [16384, 2048], P(('ep', 'tp'))
The draws below stay inside these ranges and needn't reach their ends.
Inputs may be any that keep to these rules, and one draw needn't show every extreme that they name: `routes`: each token names 2 different experts. Among the tokens of one device no expert is named more than 10 times, and in every draw some expert is named exactly 10 times by the tokens of some device.
All inputs are finite; a program needn't handle non-finite values.
Results may differ from the reference program's by a relative error of at most 0.014.
Values may be sent and summed in bfloat16 or wider, within the bound.
A program may use at most 128 MiB of HBM per device.

```python
import math
import jax
import jax.numpy as jnp
import numpy as np
from jax import lax

D = 2048
HEADS = 8
HEAD = 64
VDIM = 128
FFE = 3584
TOP = 2
TOK2_DEV = 128
SEQ = 16384
TOKENS2 = 16384
EXPERTS = 32
CAP = 10
N_EP = 32
N_TP = 4


def drawn_pairs(key):
    folded = jax.random.fold_in(key, 17)
    key_query, key_keys = jax.random.split(folded, 2)
    row_width = HEADS * 2 * HEAD
    spread = 1.32
    query_draw = jax.random.normal(key_query, (SEQ, row_width), jnp.float32) * spread
    key_draw = jax.random.normal(key_keys, (SEQ, row_width), jnp.float32) * spread
    return (jnp.clip(query_draw, -8.0, 8.0), jnp.clip(key_draw, -8.0, 8.0))


def draw_queries(key, part):
    return drawn_pairs(key)[0].astype(jnp.bfloat16)


def draw_key_rows(key, part):
    return drawn_pairs(key)[1].astype(jnp.bfloat16)


def draw_moe_input(key, part):
    folded = jax.random.fold_in(key, 23)
    key_rows_scale, key_cols_scale, key_sample = jax.random.split(folded, 3)
    row_scale = jnp.exp(jax.random.uniform(key_rows_scale, (TOKENS2, 1), jnp.float32, 0.0, math.log(10.0)))
    column_scale = jnp.exp(jax.random.uniform(key_cols_scale, (1, D), jnp.float32, 0.0, math.log(10.0)))
    sample = jax.random.normal(key_sample, (TOKENS2, D), jnp.float32)
    return jnp.clip(sample * row_scale * column_scale, -400.0, 400.0).astype(jnp.bfloat16)


def shard_levels(key, shape, cuts, least, top_value):
    factor_of, own = 1.0, jax.random.fold_in(key, 6)
    for dim, shards_of in cuts:
        draws = jnp.exp(jax.random.uniform(jax.random.fold_in(own, dim), (shards_of,), jnp.float32, least / len(cuts), top_value / len(cuts)))
        factor_of = factor_of * jnp.repeat(draws, shape[dim] // shards_of).reshape([-1 if axis == dim else 1 for axis in range(len(shape))])
    return factor_of


def assign_block(rng, own, number, rows, count, top, most, slope):
    order = jax.random.permutation(rng, count)
    crowded, usual = shares(count, rows * top, most, slope, True), shares(count, rows * top, most, slope, False)
    places = jnp.arange(count)

    def named(lengths, rotation):
        used = int((lengths > 0).sum())
        fixed = max(1, used // 4)
        shifted = fixed + (places - fixed + rotation * (used - fixed)) % max(1, count - fixed)
        return jnp.zeros((count,), jnp.int32).at[order[jnp.where(places < fixed, places, shifted)]].set(jnp.asarray(lengths, jnp.int32))

    lengths = jnp.where(number % 4 == 0, named(crowded, number // 4), named(usual, number - number // 4 - 1))
    mixed = jax.random.permutation(jax.random.fold_in(own, 3), count)
    donor, taker = mixed[0:count // 2 * 2:2], mixed[1:count // 2 * 2:2]
    room = jnp.minimum(lengths[donor] - 1, most - lengths[taker]) // 2
    room = jnp.where((donor == order[0]) | (taker == order[0]) | (lengths[taker] == 0), 0, jnp.maximum(room, 0))
    shifted = jax.random.randint(jax.random.fold_in(own, 4), (count // 2,), 0, 1 << 20) % (room + 1)
    lengths = lengths.at[donor].add(-shifted).at[taker].add(shifted)
    items = jnp.searchsorted(jnp.cumsum(lengths), jnp.arange(rows * top), side="right").astype(jnp.int32)
    table = items.reshape(top, rows).T
    table = table[jax.random.permutation(jax.random.fold_in(own, 1), rows)]
    rotation = jax.random.randint(jax.random.fold_in(own, 2), (rows, 1), 0, top)
    return jnp.take_along_axis(table, (jnp.arange(top)[None, :] + rotation) % top, axis=1)


def shares(number_of, total, most, slope, full):
    loads = [(1 << 20) // math.isqrt(rank ** slope) + 1 for rank in range(1, number_of + 1)]
    largest = most if full else min(most, max(-(-total // number_of), total * loads[0] // sum(loads)))
    least = 1 if total - largest >= number_of - 1 else 0
    counts, rest = [largest] + [least] * (number_of - 1), total - largest - least * (number_of - 1)
    while rest > 0:
        candidates = [i for i in range(1, number_of) if counts[i] < largest] or [i for i in range(1, number_of) if counts[i] < most]
        whole, left = sum([loads[i] for i in candidates]), rest
        for i in candidates:
            more = min(most - counts[i], max(1, left * loads[i] // whole), rest)
            counts[i] = counts[i] + more
            rest = rest - more
    return np.array(counts)


def normal_values(key, dims, deviation, most, cuts=(), kind=jnp.bfloat16):
    values = deviation * jax.random.normal(key, dims, jnp.float32)
    if cuts:
        values = values * shard_levels(key, dims, cuts, -0.22, 0.18)
    return jnp.clip(values, -most, most).astype(kind)


def setup_inputs(seed: int = 0) -> dict:
    seeds = jax.random.split(jax.random.key(seed), 14)
    queries = draw_queries(jax.random.fold_in(seeds[13], 71), 0)
    key_rows = draw_key_rows(jax.random.fold_in(seeds[13], 71), 0)
    value_rows = normal_values(seeds[2], (SEQ, HEADS * VDIM), 1.0, 6.0, ((0, 32), (1, 4)))
    lambdas = jnp.clip(0.3 + 0.5 * jax.random.uniform(seeds[3], (HEADS,), jnp.float32) ** shard_levels(seeds[3], (HEADS,), ((0, 4),), -0.2, 0.2), 0.3, 0.8)
    head_gain = jnp.clip(1.0 + 0.18 * jax.random.normal(seeds[4], (VDIM,), jnp.float32), 0.1, 1.9)
    out_weight = normal_values(seeds[5], (HEADS * VDIM, D), (HEADS * VDIM) ** -0.5, 0.1875, ((0, 4),))
    moe_input = draw_moe_input(jax.random.fold_in(seeds[13], 71), 0)
    moe_gain = jnp.clip(1.0 + 0.18 * jax.random.normal(seeds[7], (D,), jnp.float32), 0.1, 1.9)
    routes_keys = jax.random.split(jax.random.fold_in(seeds[8], 1), TOKENS2 // TOK2_DEV)
    routes_turns = jax.random.permutation(jax.random.fold_in(seeds[8], 3), TOKENS2 // TOK2_DEV)
    routes = jax.vmap(lambda own, number: assign_block(jax.random.fold_in(seeds[8], 2), own, number, TOK2_DEV, EXPERTS, TOP, CAP, 1))(routes_keys, routes_turns).reshape((TOKENS2, TOP))
    route_logits = normal_values(seeds[9], (TOKENS2, TOP), 1.5, 6.0, ((0, 128),), jnp.float32)
    expert_gate = normal_values(seeds[10], (EXPERTS, D, FFE), D ** -0.5, 0.125, ((0, 32), (2, 4)))
    expert_up = normal_values(seeds[11], (EXPERTS, D, FFE), D ** -0.5, 0.125, ((0, 32), (2, 4)))
    expert_down = normal_values(seeds[12], (EXPERTS, FFE, D), FFE ** -0.5, 0.09375, ((0, 32), (1, 4)))
    return dict(queries=queries, key_rows=key_rows, value_rows=value_rows, lambdas=lambdas, head_gain=head_gain, out_weight=out_weight, moe_input=moe_input, moe_gain=moe_gain, routes=routes, route_logits=route_logits, expert_gate=expert_gate, expert_up=expert_up, expert_down=expert_down)


epsilon = 1e-06
init_lambda = 0.2

def one_head(query_head, key_head, value_head, lambda_head, head_gain):
    seq_len = query_head.shape[0]
    block_rows = math.gcd(seq_len, 512)
    score_scale = HEAD ** (-0.5)
    blocks = query_head.reshape(seq_len // block_rows, block_rows, 2, HEAD)

    def one_block(query_block):
        outputs = []
        for map_index in range(2):
            scores = jnp.dot(query_block[:, map_index], key_head[:, map_index].T, preferred_element_type=jnp.float32) * score_scale
            maxima = lax.optimization_barrier(jnp.max(scores, axis=-1, keepdims=True))
            exponent = jnp.exp(scores - maxima)
            totals = lax.optimization_barrier(jnp.sum(exponent, axis=-1, keepdims=True))
            product = jnp.dot(exponent.astype(jnp.bfloat16), value_head, preferred_element_type=jnp.float32)
            outputs.append(product / totals)
        head_out = outputs[0] - lambda_head * outputs[1]
        mean_square = lax.optimization_barrier(jnp.mean(head_out * head_out, axis=-1, keepdims=True))
        return (head_out * lax.rsqrt(mean_square + epsilon) * head_gain * (1.0 - init_lambda)).astype(jnp.bfloat16)
    return lax.map(one_block, blocks).reshape(seq_len, VDIM)

def reference(queries, key_rows, value_rows, lambdas, head_gain, out_weight, moe_input, moe_gain, routes, route_logits, expert_gate, expert_up, expert_down):
    seq_len = queries.shape[0]
    query_heads = queries.reshape(seq_len, HEADS, 2, HEAD).transpose(1, 0, 2, 3)
    key_heads = key_rows.reshape(seq_len, HEADS, 2, HEAD).transpose(1, 0, 2, 3)
    value_heads = value_rows.reshape(seq_len, HEADS, VDIM).transpose(1, 0, 2)

    def head_step(packed):
        return one_head(packed[0], packed[1], packed[2], packed[3], head_gain)
    attended = lax.map(head_step, (query_heads, key_heads, value_heads, lambdas))
    group_heads = HEADS // N_TP
    weight_heads = out_weight.reshape(HEADS, VDIM, D)
    mixer_total = jnp.zeros((seq_len, D), jnp.float32)
    for group_index in range(N_TP):
        lower = group_index * group_heads
        partial_value = jnp.einsum('hqe,hed->qd', attended[lower:lower + group_heads].astype(jnp.float32), weight_heads[lower:lower + group_heads].astype(jnp.float32))
        mixer_total = mixer_total + lax.optimization_barrier(partial_value.astype(jnp.bfloat16)).astype(jnp.float32)
    mixer_out = mixer_total.astype(jnp.bfloat16)
    moe_float = moe_input.astype(jnp.float32)
    normed = (moe_float * lax.rsqrt(lax.optimization_barrier(jnp.mean(moe_float * moe_float, axis=-1, keepdims=True)) + epsilon) * moe_gain).astype(jnp.bfloat16)
    gate_weights = jax.nn.softmax(route_logits, axis=-1)
    device_count = N_EP * N_TP
    per_device = TOK2_DEV * TOP
    flat_routes = routes.reshape(device_count, per_device)
    chosen = (flat_routes[:, :, None] == jnp.arange(EXPERTS, dtype=jnp.int32)[None, None, :]).astype(jnp.int32)
    slot_rank = lax.optimization_barrier(jnp.sum((jnp.cumsum(chosen, axis=1) - chosen) * chosen, axis=2))
    device_ids = jnp.arange(device_count, dtype=jnp.int32)[:, None] * jnp.ones((1, per_device), jnp.int32)
    positions = (device_ids * CAP + slot_rank).reshape(-1).astype(jnp.int32)
    row_ids = (jnp.arange(device_count * per_device, dtype=jnp.int32) // TOP).astype(jnp.int32)
    expert_ids = flat_routes.reshape(-1).astype(jnp.int32)
    slot_table = jnp.full((EXPERTS, device_count * CAP), TOKENS2, jnp.int32).at[expert_ids, positions].set(row_ids)
    padded = jnp.concatenate([normed, jnp.zeros((1, D), jnp.bfloat16)], axis=0)
    width_part = FFE // N_TP

    def one_expert(packed):
        indices, gate_matrix, up_matrix, down_matrix = packed
        rows_in = padded[indices]
        gate_part = jnp.dot(rows_in, gate_matrix, preferred_element_type=jnp.float32)
        up_part = jnp.dot(rows_in, up_matrix, preferred_element_type=jnp.float32)
        hidden = (jax.nn.silu(gate_part) * up_part).astype(jnp.bfloat16)
        summed = jnp.zeros((rows_in.shape[0], D), jnp.float32)
        for group_index in range(N_TP):
            lower = group_index * width_part
            partial_value = jnp.dot(hidden[:, lower:lower + width_part], down_matrix[lower:lower + width_part], preferred_element_type=jnp.float32)
            summed = summed + lax.optimization_barrier(partial_value.astype(jnp.bfloat16)).astype(jnp.float32)
        return summed.astype(jnp.bfloat16)
    replies = lax.map(one_expert, (slot_table, expert_gate, expert_up, expert_down))
    picked = replies[expert_ids, positions].reshape(TOKENS2, TOP, D)
    expert_out = lax.optimization_barrier(jnp.sum(gate_weights[:, :, None] * picked.astype(jnp.float32), axis=1)).astype(jnp.bfloat16)
    return (mixer_out, expert_out)
```

```python
import functools
import jax
import jax.numpy as jnp
from jax import lax
from jax.experimental import pallas as pl
from jax.experimental.pallas import tpu as pltpu
from jax.sharding import PartitionSpec as P

F32 = jnp.float32
BF = jnp.bfloat16
epsilon = 1e-06
init_lambda = 0.2
LIM = 100.0
LOG2E = 1.4426950408889634
def attn_kernel(q_ref, kv_ref, o_ref, st_ref, acc_ref, *, nq, nblk, kb, qt):
    lane_id = lax.broadcasted_iota(jnp.int32, (256, 128), 0) // 64
    pick = (lane_id == lax.broadcasted_iota(jnp.int32, (256, 128), 1)).astype(BF)
    def norms(b, best):
        k = kv_ref[b, :kb, :].astype(F32)
        kk = jnp.dot((k * k).astype(BF), pick, preferred_element_type=F32)
        return jnp.maximum(best, jnp.max(kk, axis=0, keepdims=True))
    kmax = lax.fori_loop(0, nblk, norms, jnp.zeros((1, 128), F32))
    qf = q_ref[...].astype(F32)
    qq = jnp.sum((qf * qf).reshape(4, 64, nq), axis=1)
    bound2 = jnp.max(qq) * jnp.max(kmax) * (LOG2E * LOG2E * 1.05)
    small = bound2 < LIM * LIM
    row = lax.broadcasted_iota(jnp.int32, (128, 1), 0)
    ones = jnp.ones((16, 256), BF)

    def head_queries(h, i):
        qh = q_ref[128 * h:128 * h + 128, :]
        return jnp.where((row // 64) == i, qh, jnp.zeros_like(qh))

    @pl.when(small)
    def _():
        for h in range(2):
            qs = [head_queries(h, i) for i in range(2)]
            acc_ref[...] = jnp.zeros_like(acc_ref)
            def body(b, _):
                kh = kv_ref[b, :kb, 128 * h:128 * h + 128]
                vts = [jnp.concatenate([kv_ref[b, kb + 256 * t + 128 * h: kb + 256 * t + 128 * h + 128, :], ones], 0) for t in range(kb // 256)]
                for i in range(2):
                    for j in range(nq // qt):
                        s = jnp.dot(kh, qs[i][:, j * qt:(j + 1) * qt], preferred_element_type=F32)
                        p = jnp.exp2(s * LOG2E).astype(BF)
                        add = sum(jnp.dot(vts[t], p[256 * t:256 * t + 256], preferred_element_type=F32) for t in range(kb // 256))
                        acc_ref[i, :, j * qt:(j + 1) * qt] += add
                return 0
            lax.fori_loop(0, nblk, body, 0)
            for i in range(2):
                o_ref[2 * h + i] = acc_ref[i, :128]
                st_ref[2 * h + i] = acc_ref[i, 128:136]
                st_ref[4 + 2 * h + i] = jnp.zeros((8, nq), F32)

    @pl.when(jnp.logical_not(small))
    def _():
        for h in range(2):
            for i in range(2):
                qi = head_queries(h, i)
                for j in range(nq // qt):
                    acc_ref[i, :, j * qt:(j + 1) * qt] = jnp.zeros((144, qt), F32)
                    def body(b, m):
                        kh = kv_ref[b, :kb, 128 * h:128 * h + 128]
                        s = jnp.dot(kh, qi[:, j * qt:(j + 1) * qt], preferred_element_type=F32)
                        mn = jnp.maximum(m, jnp.max(s, axis=0, keepdims=True))
                        p = jnp.exp2((s - mn) * LOG2E).astype(BF)
                        add = 0.0
                        for t in range(kb // 256):
                            vt = jnp.concatenate([kv_ref[b, kb + 256 * t + 128 * h: kb + 256 * t + 128 * h + 128, :], ones], 0)
                            add = add + jnp.dot(vt, p[256 * t:256 * t + 256], preferred_element_type=F32)
                        acc_ref[i, :, j * qt:(j + 1) * qt] = acc_ref[i, :, j * qt:(j + 1) * qt] * jnp.exp2((m - mn) * LOG2E) + add
                        return mn
                    m = lax.fori_loop(0, nblk, body, jnp.full((1, qt), -1e30, F32))
                    sl = slice(j * qt, (j + 1) * qt)
                    o_ref[2 * h + i, :, sl] = acc_ref[i, :128, sl]
                    st_ref[2 * h + i, :, sl] = acc_ref[i, 128:136, sl]
                    st_ref[4 + 2 * h + i, :, sl] = jnp.broadcast_to(m, (8, qt))

def attention(qT, kv, qt=1024):
    nq = qT.shape[1]; nblk, kb2, _ = kv.shape; kb = kb2 // 2
    return pl.pallas_call(
        functools.partial(attn_kernel, nq=nq, nblk=nblk, kb=kb, qt=qt),
        out_shape=(jax.ShapeDtypeStruct((4, 128, nq), F32), jax.ShapeDtypeStruct((8, 8, nq), F32)),
        in_specs=[pl.BlockSpec(memory_space=pltpu.VMEM)] * 2,
        out_specs=(pl.BlockSpec(memory_space=pltpu.VMEM),) * 2,
        scratch_shapes=[pltpu.VMEM((2, 144, nq), F32)],
        compiler_params=pltpu.CompilerParams(vmem_limit_bytes=40 * 2**20),
        cost_estimate=pl.CostEstimate(flops=4 * nblk * kb * nq * 4 * 192 // 2, bytes_accessed=16 * 2**20, transcendentals=4 * nblk * kb * nq),
        name="attention",
    )(qT, kv)


def attend(queries, key_rows, value_rows, lambdas, head_gain):
    rows = queries.shape[0]
    n = lax.axis_size("ep")
    keys_t = value_rows.T
    packed = jnp.concatenate([key_rows, keys_t[:, :256], keys_t[:, 256:]], axis=0)
    groups = [[2 * k + c for k in range(n // 2)] for c in range(2)]
    kv = lax.all_gather(packed, "ep", axis_index_groups=groups, axis=0, tiled=True)
    kv = kv.reshape(n // 2, 2 * rows, 256)
    swap = [(k, k ^ 1) for k in range(n)]
    mine = (queries * jnp.asarray(0.125, BF)).T
    other = lax.ppermute(mine, "ep", swap)
    out, stats = attention(jnp.concatenate([mine, other], axis=1), kv)
    stats = stats[:, 0]
    far_out = lax.ppermute(out[:, :, rows:], "ep", swap)
    far_stats = lax.ppermute(stats[:, rows:], "ep", swap)
    near_max, far_max = stats[4:, :rows], far_stats[4:]
    top = jnp.maximum(near_max, far_max)
    near, far = jnp.exp(near_max - top), jnp.exp(far_max - top)
    totals = stats[:4, :rows] * near + far_stats[:4] * far
    maps = (out[:, :, :rows] * near[:, None] + far_out * far[:, None]) / totals[:, None]
    head_out = maps[0::2] - lambdas[:, None, None] * maps[1::2]
    mean_square = jnp.mean(head_out * head_out, axis=1, keepdims=True)
    attended = head_out * lax.rsqrt(mean_square + epsilon) * head_gain[:, None] * (1.0 - init_lambda)
    return attended.astype(BF).reshape(256, rows)


def capacity(tokens, top_count, experts):
    return max(2, (top_count * tokens * 5 + 4 * experts - 1) // (4 * experts))


def per_device(
    queries, key_rows, value_rows, lambdas, head_gain, out_weight, moe_input, moe_gain,
    routes, route_logits, expert_gate, expert_up, expert_down,
):
    model_width = out_weight.shape[1]
    attended = attend(queries, key_rows, value_rows, lambdas, head_gain)
    token_count, top_count = routes.shape
    experts_all = lax.axis_size("ep")
    slot_count = capacity(token_count, top_count, experts_all)
    moe_float = moe_input.astype(F32)
    normed = (
        moe_float
        * lax.rsqrt(jnp.mean(moe_float * moe_float, axis=-1, keepdims=True) + epsilon)
        * moe_gain
    ).astype(BF)
    gate_weights = jax.nn.softmax(route_logits, axis=-1)
    flat_routes = routes.reshape(-1)
    chosen = (flat_routes[:, None] == jnp.arange(experts_all, dtype=jnp.int32)[None, :]).astype(jnp.int32)
    slot_rank = jnp.sum((jnp.cumsum(chosen, axis=0) - chosen) * chosen, axis=1)
    slot_ids = (flat_routes * slot_count + slot_rank).reshape(token_count, top_count)
    dispatch = jnp.any(
        slot_ids[None, :, :] == jnp.arange(experts_all * slot_count, dtype=jnp.int32)[:, None, None],
        axis=-1,
    ).astype(BF)
    outgoing = jnp.dot(dispatch, normed, preferred_element_type=F32).astype(BF)
    arrived = lax.all_to_all(outgoing, "ep", split_axis=0, concat_axis=0, tiled=True)
    segment = lax.all_gather(arrived, "tp", axis=0, tiled=True)
    gate_part = jnp.dot(segment, expert_gate[0], preferred_element_type=F32)
    up_part = jnp.dot(segment, expert_up[0], preferred_element_type=F32)
    hidden = (jax.nn.silu(gate_part) * up_part).astype(BF)
    expert_part = jnp.dot(hidden, expert_down[0], preferred_element_type=F32).astype(BF)
    reply = lax.psum_scatter(expert_part, "tp", scatter_dimension=0, tiled=True)
    replies = lax.all_to_all(reply, "ep", split_axis=0, concat_axis=0, tiled=True)
    weights = jnp.sum(
        jnp.where(
            slot_ids[:, :, None] == jnp.arange(experts_all * slot_count, dtype=jnp.int32),
            gate_weights[:, :, None],
            0.0,
        ),
        axis=1,
    )
    picked = jnp.take(replies, slot_ids.reshape(-1), axis=0).reshape(token_count, top_count, model_width)
    expert_out = jnp.sum(gate_weights[:, :, None] * picked.astype(F32), axis=1).astype(BF)
    mixer_part = lax.dot_general(
        attended, out_weight, (((0,), (0,)), ((), ())), preferred_element_type=F32
    ).astype(BF)
    mixer_out = lax.psum_scatter(mixer_part, "tp", scatter_dimension=0, tiled=True)
    return (mixer_out, expert_out)


def solution(mesh):
    placed = (
        P("ep", "tp"),
        P("ep", "tp"),
        P("ep", "tp"),
        P("tp"),
        P(),
        P("tp", None),
        P(("ep", "tp"), None),
        P(),
        P(("ep", "tp"), None),
        P(("ep", "tp"), None),
        P("ep", None, "tp"),
        P("ep", None, "tp"),
        P("ep", "tp", None),
    )
    return jax.shard_map(
        per_device,
        mesh=mesh,
        in_specs=placed,
        out_specs=(P(("ep", "tp"), None), P(("ep", "tp"), None)),
        check_vma=False,
    )
```

```python
import functools
import jax
import jax.numpy as jnp
from jax import lax
from jax.experimental import pallas as pl
from jax.experimental.pallas import tpu as pltpu
from jax.sharding import PartitionSpec as P

F32 = jnp.float32
BF = jnp.bfloat16
epsilon = 1e-06
init_lambda = 0.2
LIM = 100.0
LOG2E = 1.4426950408889634
def attn_kernel(q_ref, kv_ref, o_ref, st_ref, acc_ref, *, nq, nblk, kb, qt):
    lane_id = lax.broadcasted_iota(jnp.int32, (256, 128), 0) // 64
    pick = (lane_id == lax.broadcasted_iota(jnp.int32, (256, 128), 1)).astype(BF)
    def norms(b, best):
        k = kv_ref[b, :kb, :].astype(F32)
        kk = jnp.dot((k * k).astype(BF), pick, preferred_element_type=F32)
        return jnp.maximum(best, jnp.max(kk, axis=0, keepdims=True))
    kmax = lax.fori_loop(0, nblk, norms, jnp.zeros((1, 128), F32))
    qf = q_ref[...].astype(F32)
    qq = jnp.sum((qf * qf).reshape(4, 64, nq), axis=1)
    bound2 = jnp.max(qq) * jnp.max(kmax) * (LOG2E * LOG2E * 1.05)
    small = bound2 < LIM * LIM
    row = lax.broadcasted_iota(jnp.int32, (128, 1), 0)
    ones = jnp.ones((16, 256), BF)

    def head_queries(h, i):
        qh = q_ref[128 * h:128 * h + 128, :]
        return jnp.where((row // 64) == i, qh, jnp.zeros_like(qh))

    @pl.when(small)
    def _():
        for h in range(2):
            qs = [head_queries(h, i) for i in range(2)]
            acc_ref[...] = jnp.zeros_like(acc_ref)
            def body(b, _):
                kh = kv_ref[b, :kb, 128 * h:128 * h + 128]
                vts = [jnp.concatenate([kv_ref[b, kb + 256 * t + 128 * h: kb + 256 * t + 128 * h + 128, :], ones], 0) for t in range(kb // 256)]
                for i in range(2):
                    for j in range(nq // qt):
                        s = jnp.dot(kh, qs[i][:, j * qt:(j + 1) * qt], preferred_element_type=F32)
                        p = jnp.exp2(s * LOG2E).astype(BF)
                        add = sum(jnp.dot(vts[t], p[256 * t:256 * t + 256], preferred_element_type=F32) for t in range(kb // 256))
                        acc_ref[i, :, j * qt:(j + 1) * qt] += add
                return 0
            lax.fori_loop(0, nblk, body, 0)
            for i in range(2):
                o_ref[2 * h + i] = acc_ref[i, :128]
                st_ref[2 * h + i] = acc_ref[i, 128:136]
                st_ref[4 + 2 * h + i] = jnp.zeros((8, nq), F32)

    @pl.when(jnp.logical_not(small))
    def _():
        for h in range(2):
            for i in range(2):
                qi = head_queries(h, i)
                for j in range(nq // qt):
                    acc_ref[i, :, j * qt:(j + 1) * qt] = jnp.zeros((144, qt), F32)
                    def body(b, m):
                        kh = kv_ref[b, :kb, 128 * h:128 * h + 128]
                        s = jnp.dot(kh, qi[:, j * qt:(j + 1) * qt], preferred_element_type=F32)
                        mn = jnp.maximum(m, jnp.max(s, axis=0, keepdims=True))
                        p = jnp.exp2((s - mn) * LOG2E).astype(BF)
                        add = 0.0
                        for t in range(kb // 256):
                            vt = jnp.concatenate([kv_ref[b, kb + 256 * t + 128 * h: kb + 256 * t + 128 * h + 128, :], ones], 0)
                            add = add + jnp.dot(vt, p[256 * t:256 * t + 256], preferred_element_type=F32)
                        acc_ref[i, :, j * qt:(j + 1) * qt] = acc_ref[i, :, j * qt:(j + 1) * qt] * jnp.exp2((m - mn) * LOG2E) + add
                        return mn
                    m = lax.fori_loop(0, nblk, body, jnp.full((1, qt), -1e30, F32))
                    sl = slice(j * qt, (j + 1) * qt)
                    o_ref[2 * h + i, :, sl] = acc_ref[i, :128, sl]
                    st_ref[2 * h + i, :, sl] = acc_ref[i, 128:136, sl]
                    st_ref[4 + 2 * h + i, :, sl] = jnp.broadcast_to(m, (8, qt))

def attention(qT, kv, qt=1024):
    nq = qT.shape[1]; nblk, kb2, _ = kv.shape; kb = kb2 // 2
    return pl.pallas_call(
        functools.partial(attn_kernel, nq=nq, nblk=nblk, kb=kb, qt=qt),
        out_shape=(jax.ShapeDtypeStruct((4, 128, nq), F32), jax.ShapeDtypeStruct((8, 8, nq), F32)),
        in_specs=[pl.BlockSpec(memory_space=pltpu.VMEM)] * 2,
        out_specs=(pl.BlockSpec(memory_space=pltpu.VMEM),) * 2,
        scratch_shapes=[pltpu.VMEM((2, 144, nq), F32)],
        compiler_params=pltpu.CompilerParams(vmem_limit_bytes=40 * 2**20),
        cost_estimate=pl.CostEstimate(flops=4 * nblk * kb * nq * 4 * 192 // 2, bytes_accessed=16 * 2**20, transcendentals=4 * nblk * kb * nq),
        name="attention",
    )(qT, kv)


def attend(queries, key_rows, value_rows, lambdas, head_gain):
    rows = queries.shape[0]
    n = lax.axis_size("ep")
    keys_t = value_rows.T
    packed = jnp.concatenate([key_rows, keys_t[:, :256], keys_t[:, 256:]], axis=0)
    groups = [[2 * k + c for k in range(n // 2)] for c in range(2)]
    kv = lax.all_gather(packed, "ep", axis_index_groups=groups, axis=0, tiled=True)
    kv = kv.reshape(n // 2, 2 * rows, 256)
    swap = [(k, k ^ 1) for k in range(n)]
    mine = (queries * jnp.asarray(0.125, BF)).T
    other = lax.ppermute(mine, "ep", swap)
    out, stats = attention(jnp.concatenate([mine, other], axis=1), kv)
    stats = stats[:, 0]
    far_out = lax.ppermute(out[:, :, rows:], "ep", swap)
    far_stats = lax.ppermute(stats[:, rows:], "ep", swap)
    near_max, far_max = stats[4:, :rows], far_stats[4:]
    top = jnp.maximum(near_max, far_max)
    near, far = jnp.exp(near_max - top), jnp.exp(far_max - top)
    totals = stats[:4, :rows] * near + far_stats[:4] * far
    maps = (out[:, :, :rows] * near[:, None] + far_out * far[:, None]) / totals[:, None]
    head_out = maps[0::2] - lambdas[:, None, None] * maps[1::2]
    mean_square = jnp.mean(head_out * head_out, axis=1, keepdims=True)
    attended = head_out * lax.rsqrt(mean_square + epsilon) * head_gain[:, None] * (1.0 - init_lambda)
    return attended.astype(BF).reshape(256, rows)


MESH = pl.DeviceIdType.MESH
GROUPS = 8
MAIN = 8


def front_kernel(
    main_ref, tail_ref, gate_ref, up_ref, down_ref, out_ref, seg_ref, end_ref, g_buf, u_buf, d_buf,
    own_sem, load_sem, put_send, put_recv, near_send, near_recv, far_send, far_recv,
):
    e, x = lax.axis_index("ep"), lax.axis_index("tp")
    n = main_ref.shape[0]
    width = main_ref.shape[2]
    per = n // GROUPS
    right, left = lax.rem(x + 1, 4), lax.rem(x + 3, 4)
    across = lax.rem(x + 2, 4)
    barrier = pltpu.get_barrier_semaphore()

    def greet(k, _):
        pl.semaphore_signal(barrier, inc=1, device_id=(e ^ k, x), device_id_type=MESH)
        return 0

    lax.fori_loop(1, n, greet, 0)
    for peer in (right, left, across):
        pl.semaphore_signal(barrier, inc=1, device_id=(e, peer), device_id_type=MESH)
    pl.semaphore_wait(barrier, n + 2)

    pairs = ((main_ref, seg_ref), (tail_ref, end_ref))
    own = [pltpu.make_async_copy(src.at[0], dst.at[x, 0], own_sem.at[w]) for w, (src, dst) in enumerate(pairs)]
    for c in own:
        c.start()
    for g in range(GROUPS):
        def put(k, _, g=g):
            for w, (src, dst) in enumerate(pairs):
                pltpu.make_async_remote_copy(
                    src_ref=src.at[k], dst_ref=dst.at[x, k], send_sem=put_send.at[w], recv_sem=put_recv.at[w, g],
                    device_id=(e ^ k, x), device_id_type=MESH,
                ).start()
            return 0

        lax.fori_loop(max(1, g * per), g * per + per, put, 0)
    loads = [
        pltpu.make_async_copy(src, dst, load_sem.at[k])
        for k, (src, dst) in enumerate(((gate_ref, g_buf), (up_ref, u_buf), (down_ref, d_buf)))
    ]
    for c in loads:
        c.start()
    for c in own:
        c.wait()

    def span(g):
        return pl.ds(g * per, per)

    def near(w, g, d):
        part = pairs[w][1].at[x, span(g)]
        return pltpu.make_async_remote_copy(
            src_ref=part, dst_ref=part, send_sem=near_send.at[w, d, g], recv_sem=near_recv.at[w, d, g],
            device_id=(e, right if d == 0 else left), device_id_type=MESH,
        )

    def came(w, g, d):
        part = pairs[w][1].at[left if d == 0 else right, span(g)]
        return pltpu.make_async_copy(part, part, near_recv.at[w, d, g])

    def far(w, g):
        d = g % 2
        part = pairs[w][1].at[left if d == 0 else right, span(g)]
        return pltpu.make_async_remote_copy(
            src_ref=part, dst_ref=part, send_sem=far_send.at[w, g], recv_sem=far_recv.at[w, g],
            device_id=(e, right if d == 0 else left), device_id_type=MESH,
        )

    def relay(g):
        for w in range(2):
            came(w, g, g % 2).wait()
            far(w, g).start()

    for g in range(GROUPS):
        first = 1 if g == 0 else g * per
        for w, (src, dst) in enumerate(pairs):
            landed = dst.at[x, pl.ds(first, g * per + per - first)]
            pltpu.make_async_copy(landed, landed, put_recv.at[w, g]).wait()
        for w in range(2):
            for d in range(2):
                near(w, g, d).start()
        if g >= 3:
            relay(g - 3)
    for c in loads:
        c.wait()

    def expert(t, _):
        @pl.when(t == 1)
        def _():
            for g in range(GROUPS - 3, GROUPS):
                relay(g)
            for w in range(2):
                for g in range(0, GROUPS, 2):
                    came(w, g, 1).wait()

        @pl.when(t == 2)
        def _():
            for w in range(2):
                for g in range(1, GROUPS, 2):
                    came(w, g, 0).wait()

        @pl.when(t == 3)
        def _():
            for w in range(2):
                for g in range(GROUPS):
                    part = pairs[w][1].at[across, span(g)]
                    pltpu.make_async_copy(part, part, far_recv.at[w, g]).wait()

        j = lax.rem(x + turn(t), 4)
        rows = jnp.concatenate(
            [seg_ref[j].reshape(n * MAIN, width), end_ref[j].reshape(n * 2, width)], axis=0
        )
        gate = jnp.dot(rows, g_buf[...], preferred_element_type=F32)
        up = jnp.dot(rows, u_buf[...], preferred_element_type=F32)
        hidden = (gate / (1.0 + jnp.exp(-gate)) * up).astype(BF)
        out_ref[j] = jnp.dot(hidden, d_buf[...], preferred_element_type=F32).astype(BF)
        return 0

    lax.fori_loop(0, 4, expert, 0)
    for w, (src, dst) in enumerate(pairs):
        sent = dst.at[x, pl.ds(1, n - 1)]
        pltpu.make_async_copy(sent, sent, put_send.at[w]).wait()
        for g in range(GROUPS):
            for d in range(2):
                near(w, g, d).wait_send()
            far(w, g).wait_send()


def turn(t):
    return t + (t // 2) * (1 - 2 * (t % 2))


def front(main, tail, gate, up, down):
    n, _, width = main.shape
    dma = pltpu.SemaphoreType.DMA
    hbm = pl.BlockSpec(memory_space=pl.ANY)
    return pl.pallas_call(
        front_kernel,
        out_shape=jax.ShapeDtypeStruct((4, n * (MAIN + 2), width), BF),
        in_specs=[hbm] * 5,
        out_specs=pl.BlockSpec(memory_space=pltpu.VMEM),
        scratch_shapes=[
            pltpu.VMEM((4, n, MAIN, width), BF), pltpu.VMEM((4, n, 2, width), BF),
            pltpu.VMEM(gate.shape, BF), pltpu.VMEM(up.shape, BF), pltpu.VMEM(down.shape, BF),
            dma((2,)), dma((3,)), dma((2,)), dma((2, GROUPS)), dma((2, 2, GROUPS)), dma((2, 2, GROUPS)),
            dma((2, GROUPS)), dma((2, GROUPS)),
        ],
        compiler_params=pltpu.CompilerParams(
            collective_id=0, has_side_effects=True, vmem_limit_bytes=60 * 1024 * 1024
        ),
        cost_estimate=pl.CostEstimate(flops=50 * 10**9, bytes_accessed=18 * 2**20, transcendentals=0),
        name="dispatch",
    )(main, tail, gate, up, down)


def reply_kernel(main_ref, tail_ref, got_ref, end_ref, own_sem, put_send, put_recv):
    e, x = lax.axis_index("ep"), lax.axis_index("tp")
    n = main_ref.shape[0]
    barrier = pltpu.get_barrier_semaphore()

    def greet(k, _):
        pl.semaphore_signal(barrier, inc=1, device_id=(e ^ k, x), device_id_type=MESH)
        return 0

    lax.fori_loop(1, n, greet, 0)
    pl.semaphore_wait(barrier, n - 1)
    pairs = ((main_ref, got_ref), (tail_ref, end_ref))
    own = [pltpu.make_async_copy(src.at[0], dst.at[0], own_sem.at[w]) for w, (src, dst) in enumerate(pairs)]
    for c in own:
        c.start()

    def put(k, _):
        for w, (src, dst) in enumerate(pairs):
            pltpu.make_async_remote_copy(
                src_ref=src.at[k], dst_ref=dst.at[k], send_sem=put_send.at[w], recv_sem=put_recv.at[w],
                device_id=(e ^ k, x), device_id_type=MESH,
            ).start()
        return 0

    lax.fori_loop(1, n, put, 0)
    for c in own:
        c.wait()
    for w, (src, dst) in enumerate(pairs):
        moved = dst.at[pl.ds(1, n - 1)]
        pltpu.make_async_copy(moved, moved, put_recv.at[w]).wait()
        pltpu.make_async_copy(moved, moved, put_send.at[w]).wait()


def send_back(main, tail):
    dma = pltpu.SemaphoreType.DMA
    return pl.pallas_call(
        reply_kernel,
        out_shape=(jax.ShapeDtypeStruct(main.shape, BF), jax.ShapeDtypeStruct(tail.shape, BF)),
        in_specs=[pl.BlockSpec(memory_space=pltpu.HBM)] * 2,
        out_specs=(pl.BlockSpec(memory_space=pltpu.VMEM),) * 2,
        scratch_shapes=[dma((2,)), dma((2,)), dma((2,))],
        compiler_params=pltpu.CompilerParams(
            collective_id=1, has_side_effects=True, vmem_limit_bytes=8 * 2**20
        ),
        cost_estimate=pl.CostEstimate(flops=10 * 10**9, bytes_accessed=3 * 2**20, transcendentals=0),
        name="replies",
    )(main, tail)


def per_device(
    queries, key_rows, value_rows, lambdas, head_gain, out_weight, moe_input, moe_gain,
    routes, route_logits, expert_gate, expert_up, expert_down,
):
    width = out_weight.shape[1]
    token_count, top_count = routes.shape
    n = lax.axis_size("ep")
    attended = attend(queries, key_rows, value_rows, lambdas, head_gain)
    moe_float = moe_input.astype(F32)
    normed = (
        moe_float
        * lax.rsqrt(jnp.mean(moe_float * moe_float, axis=-1, keepdims=True) + epsilon)
        * moe_gain
    ).astype(BF)
    gate_weights = jax.nn.softmax(route_logits, axis=-1)
    flat_routes = routes.reshape(-1)
    chosen = (flat_routes[:, None] == jnp.arange(n, dtype=jnp.int32)[None, :]).astype(jnp.int32)
    rank = jnp.sum((jnp.cumsum(chosen, axis=0) - chosen) * chosen, axis=1)
    step = flat_routes ^ lax.axis_index("ep")
    place = jnp.where(rank < MAIN, step * MAIN + rank, n * MAIN + step * 2 + rank - MAIN)
    place = place.reshape(token_count, top_count)
    slots = jnp.arange(n * (MAIN + 2), dtype=jnp.int32)
    dispatch = jnp.any(place[None, :, :] == slots[:, None, None], axis=-1).astype(BF)
    outgoing = jnp.dot(dispatch, normed, preferred_element_type=F32).astype(BF)
    part = front(
        outgoing[: n * MAIN].reshape(n, MAIN, width), outgoing[n * MAIN :].reshape(n, 2, width),
        expert_gate[0], expert_up[0], expert_down[0],
    )
    reply = lax.psum_scatter(part.reshape(-1, width), "tp", scatter_dimension=0, tiled=True)
    got, got_end = send_back(
        reply[: n * MAIN].reshape(n, MAIN, width), reply[n * MAIN :].reshape(n, 2, width)
    )
    weights = jnp.sum(
        jnp.where(place[:, :, None] == slots, gate_weights[:, :, None], 0.0), axis=1
    )
    high = weights.astype(BF)
    low = (weights - high.astype(F32)).astype(BF)
    both = jnp.concatenate([got.reshape(n * MAIN, width), got_end.reshape(n * 2, width)], axis=0)
    expert_out = (
        jnp.dot(high, both, preferred_element_type=F32) + jnp.dot(low, both, preferred_element_type=F32)
    ).astype(BF)
    mixer_part = lax.dot_general(
        attended, out_weight, (((0,), (0,)), ((), ())), preferred_element_type=F32
    ).astype(BF)
    mixer_out = lax.psum_scatter(mixer_part, "tp", scatter_dimension=0, tiled=True)
    return (mixer_out, expert_out)


def solution(mesh):
    placed = (
        P("ep", "tp"),
        P("ep", "tp"),
        P("ep", "tp"),
        P("tp"),
        P(),
        P("tp", None),
        P(("ep", "tp"), None),
        P(),
        P(("ep", "tp"), None),
        P(("ep", "tp"), None),
        P("ep", None, "tp"),
        P("ep", None, "tp"),
        P("ep", "tp", None),
    )
    return jax.shard_map(
        per_device,
        mesh=mesh,
        in_specs=placed,
        out_specs=(P(("ep", "tp"), None), P(("ep", "tp"), None)),
        check_vma=False,
    )
```

```python
import functools
import jax
import jax.numpy as jnp
from jax import lax
from jax.experimental import pallas as pl
from jax.experimental.pallas import tpu as pltpu
from jax.sharding import PartitionSpec as P

F32 = jnp.float32
BF = jnp.bfloat16
epsilon = 1e-06
init_lambda = 0.2
LIM = 100.0
LOG2E = 1.4426950408889634
def attn_kernel(mine_ref, far_ref, k_ref, v_ref, o_ref, st_ref, acc_ref, *, nq, nblk, kb, qt):
    def both(rows):
        return jnp.concatenate([mine_ref[rows], far_ref[rows]], axis=1)

    def other(b):
        return (b % 4) * 4 + b // 4

    lane_id = lax.broadcasted_iota(jnp.int32, (256, 128), 0) // 64
    pick = (lane_id == lax.broadcasted_iota(jnp.int32, (256, 128), 1)).astype(BF)
    def norms(b, best):
        k = k_ref[b].astype(F32)
        kk = jnp.dot((k * k).astype(BF), pick, preferred_element_type=F32)
        return jnp.maximum(best, jnp.max(kk, axis=0, keepdims=True))
    kmax = lax.fori_loop(0, nblk, norms, jnp.zeros((1, 128), F32))
    qf = both(slice(0, 256)).astype(F32)
    qq = jnp.sum((qf * qf).reshape(4, 64, nq), axis=1)
    bound2 = jnp.max(qq) * jnp.max(kmax) * (LOG2E * LOG2E * 1.05)
    small = bound2 < LIM * LIM
    row = lax.broadcasted_iota(jnp.int32, (128, 1), 0)
    ones = jnp.ones((16, 256), BF)

    def head_queries(h, i):
        qh = both(slice(128 * h, 128 * h + 128))
        return jnp.where((row // 64) == i, qh, jnp.zeros_like(qh))

    @pl.when(small)
    def _():
        for h in range(2):
            qs = [head_queries(h, i) for i in range(2)]
            acc_ref[...] = jnp.zeros_like(acc_ref)
            def body(b, _):
                kh = k_ref[b, :, 128 * h:128 * h + 128]
                vts = [jnp.concatenate([v_ref[other(b), 256 * t + 128 * h: 256 * t + 128 * h + 128, :], ones], 0) for t in range(kb // 256)]
                for i in range(2):
                    for j in range(nq // qt):
                        s = jnp.dot(kh, qs[i][:, j * qt:(j + 1) * qt], preferred_element_type=F32)
                        p = jnp.exp2(s * LOG2E).astype(BF)
                        add = sum(jnp.dot(vts[t], p[256 * t:256 * t + 256], preferred_element_type=F32) for t in range(kb // 256))
                        acc_ref[i, :, j * qt:(j + 1) * qt] += add
                return 0
            lax.fori_loop(0, nblk, body, 0)
            for i in range(2):
                o_ref[2 * h + i] = acc_ref[i, :128]
                st_ref[2 * h + i] = acc_ref[i, 128:136]
                st_ref[4 + 2 * h + i] = jnp.zeros((8, nq), F32)

    @pl.when(jnp.logical_not(small))
    def _():
        for h in range(2):
            for i in range(2):
                qi = head_queries(h, i)
                for j in range(nq // qt):
                    acc_ref[i, :, j * qt:(j + 1) * qt] = jnp.zeros((144, qt), F32)
                    def body(b, m):
                        kh = k_ref[b, :, 128 * h:128 * h + 128]
                        s = jnp.dot(kh, qi[:, j * qt:(j + 1) * qt], preferred_element_type=F32)
                        mn = jnp.maximum(m, jnp.max(s, axis=0, keepdims=True))
                        p = jnp.exp2((s - mn) * LOG2E).astype(BF)
                        add = 0.0
                        for t in range(kb // 256):
                            vt = jnp.concatenate([v_ref[other(b), 256 * t + 128 * h: 256 * t + 128 * h + 128, :], ones], 0)
                            add = add + jnp.dot(vt, p[256 * t:256 * t + 256], preferred_element_type=F32)
                        acc_ref[i, :, j * qt:(j + 1) * qt] = acc_ref[i, :, j * qt:(j + 1) * qt] * jnp.exp2((m - mn) * LOG2E) + add
                        return mn
                    m = lax.fori_loop(0, nblk, body, jnp.full((1, qt), -1e30, F32))
                    sl = slice(j * qt, (j + 1) * qt)
                    o_ref[2 * h + i, :, sl] = acc_ref[i, :128, sl]
                    st_ref[2 * h + i, :, sl] = acc_ref[i, 128:136, sl]
                    st_ref[4 + 2 * h + i, :, sl] = jnp.broadcast_to(m, (8, qt))

def attention(mine, far, keys, values, qt=1024):
    nq = 2 * mine.shape[1]
    nblk, kb, _ = keys.shape
    return pl.pallas_call(
        functools.partial(attn_kernel, nq=nq, nblk=nblk, kb=kb, qt=qt),
        out_shape=(jax.ShapeDtypeStruct((4, 128, nq), F32), jax.ShapeDtypeStruct((8, 8, nq), F32)),
        in_specs=[pl.BlockSpec(memory_space=pltpu.VMEM)] * 4,
        out_specs=(pl.BlockSpec(memory_space=pltpu.VMEM),) * 2,
        scratch_shapes=[pltpu.VMEM((2, 144, nq), F32)],
        compiler_params=pltpu.CompilerParams(vmem_limit_bytes=40 * 2**20),
        cost_estimate=pl.CostEstimate(flops=4 * nblk * kb * nq * 4 * 192 // 2, bytes_accessed=16 * 2**20, transcendentals=4 * nblk * kb * nq),
        name="attention",
    )(mine, far, keys, values)


def attend(mine, far, keys, values, lambdas, head_gain):
    rows = mine.shape[1]
    n = lax.axis_size("ep")
    swap = [(k, k ^ 1) for k in range(n)]
    out, stats = attention(mine, far, keys, values)
    stats = stats[:, 0]
    far_out = lax.ppermute(out[:, :, rows:], "ep", swap)
    far_stats = lax.ppermute(stats[:, rows:], "ep", swap)
    near_max, far_max = stats[4:, :rows], far_stats[4:]
    top = jnp.maximum(near_max, far_max)
    near, far = jnp.exp(near_max - top), jnp.exp(far_max - top)
    totals = stats[:4, :rows] * near + far_stats[:4] * far
    maps = (out[:, :, :rows] * near[:, None] + far_out * far[:, None]) / totals[:, None]
    head_out = maps[0::2] - lambdas[:, None, None] * maps[1::2]
    mean_square = jnp.mean(head_out * head_out, axis=1, keepdims=True)
    attended = head_out * lax.rsqrt(mean_square + epsilon) * head_gain[:, None] * (1.0 - init_lambda)
    return attended.astype(BF).reshape(256, rows)


MESH = pl.DeviceIdType.MESH
GROUPS = 8
MAIN = 8


def front_kernel(
    main_ref, tail_ref, gate_ref, up_ref, down_ref, key_ref, value_ref, mine_ref,
    out_ref, keys_ref, values_ref, far_ref, seg_ref, end_ref, g_buf, u_buf, d_buf,
    own_sem, load_sem, put_send, put_recv, near_send, near_recv, far_send, far_recv,
    home_sem, swap_sem, one_send, one_recv, onef_send, onef_recv, two_send, two_recv, twof_send, twof_recv,
):
    e, x = lax.axis_index("ep"), lax.axis_index("tp")
    n = main_ref.shape[0]
    width = main_ref.shape[2]
    per = n // GROUPS
    right, left = lax.rem(x + 1, 4), lax.rem(x + 3, 4)
    across = lax.rem(x + 2, 4)
    barrier = pltpu.get_barrier_semaphore()

    core, y, z = lax.rem(e, 2), lax.rem(e // 2, 4), e // 8

    def chip(dz, dy):
        return (lax.rem(z + dz, 4) * 4 + lax.rem(y + dy, 4)) * 2 + core, x

    half = key_ref.shape[0] // 2
    home = [
        pltpu.make_async_copy(key_ref, keys_ref.at[z, y], home_sem.at[0]),
        pltpu.make_async_copy(value_ref, values_ref.at[y, z], home_sem.at[1]),
    ]
    swap = pltpu.make_async_remote_copy(
        src_ref=mine_ref, dst_ref=far_ref, send_sem=swap_sem.at[0], recv_sem=swap_sem.at[1],
        device_id=(e ^ 1, x), device_id_type=MESH,
    )
    ends = (keys_ref, values_ref)
    firsts = (key_ref, value_ref)
    inner, outer = (y, z), (z, y)

    def along(w, step, second):
        return chip(step, 0) if (w == 0) == second else chip(0, step)

    def hop(src, dst, sems, w, step, second):
        return pltpu.make_async_remote_copy(
            src_ref=src, dst_ref=dst, send_sem=sems[0], recv_sem=sems[1],
            device_id=along(w, step, second), device_id_type=MESH,
        )

    def rows_of(g):
        return pl.ds(g * half, half)

    def arrival(dst, sem):
        return pltpu.make_async_copy(dst, dst, sem)

    def one_near(w, g, d):
        dst = ends[w].at[outer[w], inner[w], rows_of(g)]
        return hop(firsts[w].at[rows_of(g)], dst, (one_send.at[w, d, g], one_recv.at[w, d, g]), w, 1 if d == 0 else 3, False)

    def one_slot(w, g, step):
        return ends[w].at[outer[w], lax.rem(inner[w] + step, 4), rows_of(g)]

    def one_came(w, g, d):
        return arrival(one_slot(w, g, 3 if d == 0 else 1), one_recv.at[w, d, g])

    def one_far(w, g):
        part = one_slot(w, g, 3 if g == 0 else 1)
        return hop(part, part, (onef_send.at[w, g], onef_recv.at[w, g]), w, 1 if g == 0 else 3, False)

    def two_slot(w, r, step):
        return ends[w].at[lax.rem(outer[w] + step, 4), lax.rem(inner[w] + r, 4)]

    def two_near(w, r, d):
        src = firsts[w] if r == 0 else two_slot(w, r, 0)
        return hop(src, two_slot(w, r, 0), (two_send.at[w, d, r], two_recv.at[w, d, r]), w, 1 if d == 0 else 3, True)

    def two_came(w, r, d):
        return arrival(two_slot(w, r, 3 if d == 0 else 1), two_recv.at[w, d, r])

    def via(r):
        return 0 if r in (0, 1) else 1

    def two_far(w, r):
        d = via(r)
        part = two_slot(w, r, 3 if d == 0 else 1)
        return hop(part, part, (twof_send.at[w, r], twof_recv.at[w, r]), w, 1 if d == 0 else 3, True)

    def spread_first():
        for c in home:
            c.start()
        for w in range(2):
            for g in range(2):
                for d in range(2):
                    one_near(w, g, d).start()
        for w in range(2):
            for d in range(2):
                two_near(w, 0, d).start()

    def spread_near():
        for w in range(2):
            for g in range(2):
                one_came(w, g, g).wait()
                one_far(w, g).start()
        for r in (1, 3):
            for w in range(2):
                one_came(w, 1 - (0 if r == 3 else 1), 0 if r == 3 else 1).wait()
                for d in range(2):
                    two_near(w, r, d).start()

    def spread_across():
        for w in range(2):
            for g in range(2):
                arrival(one_slot(w, g, 2), onef_recv.at[w, g]).wait()
            for d in range(2):
                two_near(w, 2, d).start()

    def spread_relay(r):
        for w in range(2):
            two_came(w, r, via(r)).wait()
            two_far(w, r).start()

    def spread_end():
        for w in range(2):
            home[w].wait()
            for r in range(4):
                two_came(w, r, 1 - via(r)).wait()
                arrival(two_slot(w, r, 2), twof_recv.at[w, r]).wait()
                two_far(w, r).wait_send()
                for d in range(2):
                    two_near(w, r, d).wait_send()
            for g in range(2):
                one_far(w, g).wait_send()
                for d in range(2):
                    one_near(w, g, d).wait_send()
        swap.wait()

    def greet(k, _):
        pl.semaphore_signal(barrier, inc=1, device_id=(e ^ k, x), device_id_type=MESH)
        return 0

    lax.fori_loop(1, n, greet, 0)
    for peer in (right, left, across):
        pl.semaphore_signal(barrier, inc=1, device_id=(e, peer), device_id_type=MESH)
    pl.semaphore_wait(barrier, n + 2)

    pairs = ((main_ref, seg_ref), (tail_ref, end_ref))
    own = [pltpu.make_async_copy(src.at[0], dst.at[x, 0], own_sem.at[w]) for w, (src, dst) in enumerate(pairs)]
    for c in own:
        c.start()
    for g in range(GROUPS):
        def put(k, _, g=g):
            for w, (src, dst) in enumerate(pairs):
                pltpu.make_async_remote_copy(
                    src_ref=src.at[k], dst_ref=dst.at[x, k], send_sem=put_send.at[w], recv_sem=put_recv.at[w, g],
                    device_id=(e ^ k, x), device_id_type=MESH,
                ).start()
            return 0

        lax.fori_loop(max(1, g * per), g * per + per, put, 0)
    swap.start()
    spread_first()
    loads = [
        pltpu.make_async_copy(src, dst, load_sem.at[k])
        for k, (src, dst) in enumerate(((gate_ref, g_buf), (up_ref, u_buf), (down_ref, d_buf)))
    ]
    for c in loads:
        c.start()
    for c in own:
        c.wait()

    def span(g):
        return pl.ds(g * per, per)

    def near(w, g, d):
        part = pairs[w][1].at[x, span(g)]
        return pltpu.make_async_remote_copy(
            src_ref=part, dst_ref=part, send_sem=near_send.at[w, d, g], recv_sem=near_recv.at[w, d, g],
            device_id=(e, right if d == 0 else left), device_id_type=MESH,
        )

    def came(w, g, d):
        part = pairs[w][1].at[left if d == 0 else right, span(g)]
        return pltpu.make_async_copy(part, part, near_recv.at[w, d, g])

    def far(w, g):
        d = g % 2
        part = pairs[w][1].at[left if d == 0 else right, span(g)]
        return pltpu.make_async_remote_copy(
            src_ref=part, dst_ref=part, send_sem=far_send.at[w, g], recv_sem=far_recv.at[w, g],
            device_id=(e, right if d == 0 else left), device_id_type=MESH,
        )

    def relay(g):
        for w in range(2):
            came(w, g, g % 2).wait()
            far(w, g).start()

    for g in range(GROUPS):
        first = 1 if g == 0 else g * per
        for w, (src, dst) in enumerate(pairs):
            landed = dst.at[x, pl.ds(first, g * per + per - first)]
            pltpu.make_async_copy(landed, landed, put_recv.at[w, g]).wait()
        for w in range(2):
            for d in range(2):
                near(w, g, d).start()
        if g >= 3:
            relay(g - 3)
    for c in loads:
        c.wait()

    def expert(t, _):
        @pl.when(t == 1)
        def _():
            for g in range(GROUPS - 3, GROUPS):
                relay(g)
            spread_near()
            spread_relay(0)
            for w in range(2):
                for g in range(0, GROUPS, 2):
                    came(w, g, 1).wait()

        @pl.when(t == 2)
        def _():
            spread_across()
            spread_relay(1)
            for w in range(2):
                for g in range(1, GROUPS, 2):
                    came(w, g, 0).wait()

        @pl.when(t == 3)
        def _():
            spread_relay(3)
            spread_relay(2)
            for w in range(2):
                for g in range(GROUPS):
                    part = pairs[w][1].at[across, span(g)]
                    pltpu.make_async_copy(part, part, far_recv.at[w, g]).wait()

        j = lax.rem(x + turn(t), 4)
        rows = jnp.concatenate(
            [seg_ref[j].reshape(n * MAIN, width), end_ref[j].reshape(n * 2, width)], axis=0
        )
        gate = jnp.dot(rows, g_buf[...], preferred_element_type=F32)
        up = jnp.dot(rows, u_buf[...], preferred_element_type=F32)
        hidden = (gate / (1.0 + jnp.exp(-gate)) * up).astype(BF)
        out_ref[j] = jnp.dot(hidden, d_buf[...], preferred_element_type=F32).astype(BF)
        return 0

    lax.fori_loop(0, 4, expert, 0)
    spread_end()
    for w, (src, dst) in enumerate(pairs):
        sent = dst.at[x, pl.ds(1, n - 1)]
        pltpu.make_async_copy(sent, sent, put_send.at[w]).wait()
        for g in range(GROUPS):
            for d in range(2):
                near(w, g, d).wait_send()
            far(w, g).wait_send()


def turn(t):
    return t + (t // 2) * (1 - 2 * (t % 2))


def front(main, tail, gate, up, down, key, value, mine):
    n, _, width = main.shape
    dma = pltpu.SemaphoreType.DMA
    hbm = pl.BlockSpec(memory_space=pl.ANY)
    return pl.pallas_call(
        front_kernel,
        out_shape=(
            jax.ShapeDtypeStruct((4, n * (MAIN + 2), width), BF),
            jax.ShapeDtypeStruct((4, 4, *key.shape), BF),
            jax.ShapeDtypeStruct((4, 4, *value.shape), BF),
            jax.ShapeDtypeStruct(mine.shape, BF),
        ),
        in_specs=[hbm] * 8,
        out_specs=(pl.BlockSpec(memory_space=pltpu.VMEM), hbm, hbm, hbm),
        scratch_shapes=[
            pltpu.VMEM((4, n, MAIN, width), BF), pltpu.VMEM((4, n, 2, width), BF),
            pltpu.VMEM(gate.shape, BF), pltpu.VMEM(up.shape, BF), pltpu.VMEM(down.shape, BF),
            dma((2,)), dma((3,)), dma((2,)), dma((2, GROUPS)), dma((2, 2, GROUPS)), dma((2, 2, GROUPS)),
            dma((2, GROUPS)), dma((2, GROUPS)),
            dma((2,)), dma((2,)), dma((2, 2, 2)), dma((2, 2, 2)), dma((2, 2)), dma((2, 2)),
            dma((2, 2, 4)), dma((2, 2, 4)), dma((2, 4)), dma((2, 4)),
        ],
        compiler_params=pltpu.CompilerParams(
            collective_id=0, has_side_effects=True, vmem_limit_bytes=60 * 1024 * 1024
        ),
        cost_estimate=pl.CostEstimate(flops=50 * 10**9, bytes_accessed=18 * 2**20, transcendentals=0),
        name="dispatch",
    )(main, tail, gate, up, down, key, value, mine)


def reply_kernel(main_ref, tail_ref, got_ref, end_ref, own_sem, put_send, put_recv):
    e, x = lax.axis_index("ep"), lax.axis_index("tp")
    n = main_ref.shape[0]
    barrier = pltpu.get_barrier_semaphore()

    def greet(k, _):
        pl.semaphore_signal(barrier, inc=1, device_id=(e ^ k, x), device_id_type=MESH)
        return 0

    lax.fori_loop(1, n, greet, 0)
    pl.semaphore_wait(barrier, n - 1)
    pairs = ((main_ref, got_ref), (tail_ref, end_ref))
    own = [pltpu.make_async_copy(src.at[0], dst.at[0], own_sem.at[w]) for w, (src, dst) in enumerate(pairs)]
    for c in own:
        c.start()

    def put(k, _):
        for w, (src, dst) in enumerate(pairs):
            pltpu.make_async_remote_copy(
                src_ref=src.at[k], dst_ref=dst.at[k], send_sem=put_send.at[w], recv_sem=put_recv.at[w],
                device_id=(e ^ k, x), device_id_type=MESH,
            ).start()
        return 0

    lax.fori_loop(1, n, put, 0)
    for c in own:
        c.wait()
    for w, (src, dst) in enumerate(pairs):
        moved = dst.at[pl.ds(1, n - 1)]
        pltpu.make_async_copy(moved, moved, put_recv.at[w]).wait()
        pltpu.make_async_copy(moved, moved, put_send.at[w]).wait()


def send_back(main, tail):
    dma = pltpu.SemaphoreType.DMA
    return pl.pallas_call(
        reply_kernel,
        out_shape=(jax.ShapeDtypeStruct(main.shape, BF), jax.ShapeDtypeStruct(tail.shape, BF)),
        in_specs=[pl.BlockSpec(memory_space=pltpu.HBM)] * 2,
        out_specs=(pl.BlockSpec(memory_space=pltpu.VMEM),) * 2,
        scratch_shapes=[dma((2,)), dma((2,)), dma((2,))],
        compiler_params=pltpu.CompilerParams(
            collective_id=1, has_side_effects=True, vmem_limit_bytes=8 * 2**20
        ),
        cost_estimate=pl.CostEstimate(flops=10 * 10**9, bytes_accessed=3 * 2**20, transcendentals=0),
        name="replies",
    )(main, tail)


def per_device(
    queries, key_rows, value_rows, lambdas, head_gain, out_weight, moe_input, moe_gain,
    routes, route_logits, expert_gate, expert_up, expert_down,
):
    width = out_weight.shape[1]
    token_count, top_count = routes.shape
    n = lax.axis_size("ep")
    moe_float = moe_input.astype(F32)
    normed = (
        moe_float
        * lax.rsqrt(jnp.mean(moe_float * moe_float, axis=-1, keepdims=True) + epsilon)
        * moe_gain
    ).astype(BF)
    gate_weights = jax.nn.softmax(route_logits, axis=-1)
    flat_routes = routes.reshape(-1)
    chosen = (flat_routes[:, None] == jnp.arange(n, dtype=jnp.int32)[None, :]).astype(jnp.int32)
    rank = jnp.sum((jnp.cumsum(chosen, axis=0) - chosen) * chosen, axis=1)
    step = flat_routes ^ lax.axis_index("ep")
    place = jnp.where(rank < MAIN, step * MAIN + rank, n * MAIN + step * 2 + rank - MAIN)
    place = place.reshape(token_count, top_count)
    slots = jnp.arange(n * (MAIN + 2), dtype=jnp.int32)
    dispatch = jnp.any(place[None, :, :] == slots[:, None, None], axis=-1).astype(BF)
    outgoing = jnp.dot(dispatch, normed, preferred_element_type=F32).astype(BF)
    mine = (queries * jnp.asarray(0.125, BF)).T
    values_t = value_rows.T
    value = jnp.concatenate([values_t[:, :256], values_t[:, 256:]], axis=0)
    part, keys, values, far = front(
        outgoing[: n * MAIN].reshape(n, MAIN, width), outgoing[n * MAIN :].reshape(n, 2, width),
        expert_gate[0], expert_up[0], expert_down[0], key_rows, value, mine,
    )
    attended = attend(
        mine, far, keys.reshape(16, 512, 256), values.reshape(16, 512, 256), lambdas, head_gain
    )
    reply = lax.psum_scatter(part.reshape(-1, width), "tp", scatter_dimension=0, tiled=True)
    got, got_end = send_back(
        reply[: n * MAIN].reshape(n, MAIN, width), reply[n * MAIN :].reshape(n, 2, width)
    )
    weights = jnp.sum(
        jnp.where(place[:, :, None] == slots, gate_weights[:, :, None], 0.0), axis=1
    )
    high = weights.astype(BF)
    low = (weights - high.astype(F32)).astype(BF)
    both = jnp.concatenate([got.reshape(n * MAIN, width), got_end.reshape(n * 2, width)], axis=0)
    expert_out = (
        jnp.dot(high, both, preferred_element_type=F32) + jnp.dot(low, both, preferred_element_type=F32)
    ).astype(BF)
    mixer_part = lax.dot_general(
        attended, out_weight, (((0,), (0,)), ((), ())), preferred_element_type=F32
    ).astype(BF)
    mixer_out = lax.psum_scatter(mixer_part, "tp", scatter_dimension=0, tiled=True)
    return (mixer_out, expert_out)


def solution(mesh):
    placed = (
        P("ep", "tp"),
        P("ep", "tp"),
        P("ep", "tp"),
        P("tp"),
        P(),
        P("tp", None),
        P(("ep", "tp"), None),
        P(),
        P(("ep", "tp"), None),
        P(("ep", "tp"), None),
        P("ep", None, "tp"),
        P("ep", None, "tp"),
        P("ep", "tp", None),
    )
    return jax.shard_map(
        per_device,
        mesh=mesh,
        in_specs=placed,
        out_specs=(P(("ep", "tp"), None), P(("ep", "tp"), None)),
        check_vma=False,
    )
```

```python
import functools
import jax
import jax.numpy as jnp
from jax import lax
from jax.experimental import pallas as pl
from jax.experimental.pallas import tpu as pltpu
from jax.sharding import PartitionSpec as P

F32 = jnp.float32
BF = jnp.bfloat16
epsilon = 1e-06
init_lambda = 0.2
LOG2E = 1.4426950408889634
MESH = pl.DeviceIdType.MESH
GROUPS = 8
MAIN = 8
VM = 60 * 1024 * 1024


def whole_kernel(
    main_ref, tail_ref, gate_ref, up_ref, down_ref, key_ref, value_ref, mine_ref, ow_ref, lam_ref, gain_ref,
    mixer_ref, got_ref, last_ref,
    seg_ref, end_ref, g_buf, u_buf, d_buf, part_ref, keys_ref, values_ref, far_ref, near_ref, w_buf,
    ra_ref, rl_ref, rs_ref, rep_ref, tip_ref, acc_ref, max_ref, s_ref, swap_ref,
    mp_ref, ma_ref, ml_ref, ms_ref,
    own_sem, load_sem, put_send, put_recv, near_send, near_recv, far_send, far_recv,
    home_sem, swap_sem, one_send, one_recv, onef_send, onef_recv, two_send, two_recv, twof_send, twof_recv,
    rs_send, rs_recv, mix_send, mix_recv, rep_send, rep_recv, out_sem,
):
    e, x = lax.axis_index("ep"), lax.axis_index("tp")
    n = main_ref.shape[0]
    width = main_ref.shape[2]
    per = n // GROUPS
    right, left = lax.rem(x + 1, 4), lax.rem(x + 3, 4)
    across = lax.rem(x + 2, 4)
    barrier = pltpu.get_barrier_semaphore()
    core, y, z = lax.rem(e, 2), lax.rem(e // 2, 4), e // 8

    def chip(dz, dy):
        return (lax.rem(z + dz, 4) * 4 + lax.rem(y + dy, 4)) * 2 + core, x

    half = key_ref.shape[0] // 2
    home = [
        pltpu.make_async_copy(key_ref, keys_ref.at[z, y], home_sem.at[0]),
        pltpu.make_async_copy(value_ref, values_ref.at[y, z], home_sem.at[1]),
    ]
    swap = pltpu.make_async_remote_copy(
        src_ref=mine_ref, dst_ref=far_ref, send_sem=swap_sem.at[0], recv_sem=swap_sem.at[1],
        device_id=(e ^ 1, x), device_id_type=MESH,
    )
    ends = (keys_ref, values_ref)
    firsts = (key_ref, value_ref)
    inner, outer = (y, z), (z, y)

    def along(w, step, second):
        return chip(step, 0) if (w == 0) == second else chip(0, step)

    def hop(src, dst, sems, w, step, second):
        return pltpu.make_async_remote_copy(
            src_ref=src, dst_ref=dst, send_sem=sems[0], recv_sem=sems[1],
            device_id=along(w, step, second), device_id_type=MESH,
        )

    def rows_of(g):
        return pl.ds(g * half, half)

    def arrival(dst, sem):
        return pltpu.make_async_copy(dst, dst, sem)

    def one_near(w, g, d):
        dst = ends[w].at[outer[w], inner[w], rows_of(g)]
        return hop(firsts[w].at[rows_of(g)], dst, (one_send.at[w, d, g], one_recv.at[w, d, g]), w, 1 if d == 0 else 3, False)

    def one_slot(w, g, step):
        return ends[w].at[outer[w], lax.rem(inner[w] + step, 4), rows_of(g)]

    def one_came(w, g, d):
        return arrival(one_slot(w, g, 3 if d == 0 else 1), one_recv.at[w, d, g])

    def one_far(w, g):
        part = one_slot(w, g, 3 if g == 0 else 1)
        return hop(part, part, (onef_send.at[w, g], onef_recv.at[w, g]), w, 1 if g == 0 else 3, False)

    def two_slot(w, r, step):
        return ends[w].at[lax.rem(outer[w] + step, 4), lax.rem(inner[w] + r, 4)]

    def two_near(w, r, d):
        src = firsts[w] if r == 0 else two_slot(w, r, 0)
        return hop(src, two_slot(w, r, 0), (two_send.at[w, d, r], two_recv.at[w, d, r]), w, 1 if d == 0 else 3, True)

    def two_came(w, r, d):
        return arrival(two_slot(w, r, 3 if d == 0 else 1), two_recv.at[w, d, r])

    def via(r):
        return 0 if r in (0, 1) else 1

    def two_far(w, r):
        d = via(r)
        part = two_slot(w, r, 3 if d == 0 else 1)
        return hop(part, part, (twof_send.at[w, r], twof_recv.at[w, r]), w, 1 if d == 0 else 3, True)

    def spread_first():
        for w in range(2):
            for g in range(2):
                for d in range(2):
                    one_near(w, g, d).start()
        for w in range(2):
            for d in range(2):
                two_near(w, 0, d).start()

    def spread_near():
        for w in range(2):
            for g in range(2):
                one_came(w, g, g).wait()
                one_far(w, g).start()
        for r in (1, 3):
            for w in range(2):
                one_came(w, 1 - (0 if r == 3 else 1), 0 if r == 3 else 1).wait()
                for d in range(2):
                    two_near(w, r, d).start()

    def spread_across():
        for w in range(2):
            for g in range(2):
                arrival(one_slot(w, g, 2), onef_recv.at[w, g]).wait()
            for d in range(2):
                two_near(w, 2, d).start()

    def spread_relay(r):
        for w in range(2):
            two_came(w, r, via(r)).wait()
            two_far(w, r).start()

    def greet(k, _):
        pl.semaphore_signal(barrier, inc=1, device_id=(e ^ k, x), device_id_type=MESH)
        return 0

    lax.fori_loop(1, n, greet, 0)
    for peer in (right, left, across):
        pl.semaphore_signal(barrier, inc=1, device_id=(e, peer), device_id_type=MESH)
    pl.semaphore_wait(barrier, n + 2)

    pairs = ((main_ref, seg_ref), (tail_ref, end_ref))
    own = [pltpu.make_async_copy(src.at[0], dst.at[x, 0], own_sem.at[w]) for w, (src, dst) in enumerate(pairs)]
    for c in own:
        c.start()
    for g in range(GROUPS):
        def put(k, _, g=g):
            for w, (src, dst) in enumerate(pairs):
                pltpu.make_async_remote_copy(
                    src_ref=src.at[k], dst_ref=dst.at[x, k], send_sem=put_send.at[w], recv_sem=put_recv.at[w, g],
                    device_id=(e ^ k, x), device_id_type=MESH,
                ).start()
            return 0

        lax.fori_loop(max(1, g * per), g * per + per, put, 0)
    swap.start()
    loads = [
        pltpu.make_async_copy(src, dst, load_sem.at[k])
        for k, (src, dst) in enumerate(
            ((gate_ref, g_buf), (up_ref, u_buf), (down_ref, d_buf), (mine_ref, near_ref), (ow_ref, w_buf))
        )
    ]
    for c in loads + home:
        c.start()
    for c in own:
        c.wait()

    def span(g):
        return pl.ds(g * per, per)

    def near(w, g, d):
        part = pairs[w][1].at[x, span(g)]
        return pltpu.make_async_remote_copy(
            src_ref=part, dst_ref=part, send_sem=near_send.at[w, d, g], recv_sem=near_recv.at[w, d, g],
            device_id=(e, right if d == 0 else left), device_id_type=MESH,
        )

    def came(w, g, d):
        part = pairs[w][1].at[left if d == 0 else right, span(g)]
        return pltpu.make_async_copy(part, part, near_recv.at[w, d, g])

    def far(w, g):
        d = g % 2
        part = pairs[w][1].at[left if d == 0 else right, span(g)]
        return pltpu.make_async_remote_copy(
            src_ref=part, dst_ref=part, send_sem=far_send.at[w, g], recv_sem=far_recv.at[w, g],
            device_id=(e, right if d == 0 else left), device_id_type=MESH,
        )

    def relay(g):
        for w in range(2):
            came(w, g, g % 2).wait()
            far(w, g).start()

    for g in range(GROUPS):
        first = 1 if g == 0 else g * per
        for w, (src, dst) in enumerate(pairs):
            landed = dst.at[x, pl.ds(first, g * per + per - first)]
            pltpu.make_async_copy(landed, landed, put_recv.at[w, g]).wait()
        for w in range(2):
            for d in range(2):
                near(w, g, d).start()
    spread_first()
    for g in range(GROUPS - 2):
        relay(g)
    for c in loads:
        c.wait()

    def scatter(block, half, a_ref, l_ref, t_ref, sends, recvs):
        def piece(j, hh):
            return block.at[j, pl.ds(hh * half, half)]

        def move(src, dst, k, d):
            return pltpu.make_async_remote_copy(
                src_ref=src, dst_ref=dst, send_sem=sends.at[k, d], recv_sem=recvs.at[k, d],
                device_id=(e, right if d == 0 else left), device_id_type=MESH,
            )

        def away(d):
            return move(piece(across, d), a_ref.at[d], 0, d)

        def plain(d):
            return move(piece(right if d == 0 else left, 1 - d), l_ref.at[d, 1 - d], 1, d)

        def summed(d):
            return move(t_ref.at[d], l_ref.at[d, d], 2, d)

        def join(d):
            away(d).wait_recv()
            j = right if d == 0 else left
            t_ref[d] = (a_ref[d].astype(F32) + block[j, pl.ds(d * half, half), :].astype(F32)).astype(BF)
            summed(d).start()

        def total(hh):
            return (
                block[x, pl.ds(hh * half, half), :].astype(F32) + l_ref[0, hh].astype(F32) + l_ref[1, hh].astype(F32)
            ).astype(BF)

        def landed():
            for d in range(2):
                plain(d).wait_recv()
                summed(d).wait_recv()

        def done():
            for d in range(2):
                away(d).wait_send()
                plain(d).wait_send()
                summed(d).wait_send()

        return away, plain, join, total, landed, done

    rows = n * (MAIN + 2)
    rs_away, rs_plain, rs_join, rs_total, rs_landed, rs_done = scatter(
        part_ref, rows // 2, ra_ref, rl_ref, rs_ref, rs_send, rs_recv
    )

    def expert(t, _):
        @pl.when(t == 1)
        def _():
            for g in range(GROUPS - 2, GROUPS):
                relay(g)
            for w in range(2):
                for g in range(0, GROUPS, 2):
                    came(w, g, 1).wait()

        @pl.when(t == 2)
        def _():
            rs_plain(0).start()
            for w in range(2):
                for g in range(1, GROUPS, 2):
                    came(w, g, 0).wait()
            spread_near()

        @pl.when(t == 3)
        def _():
            rs_plain(1).start()
            spread_across()
            for w in range(2):
                for g in range(GROUPS):
                    part = pairs[w][1].at[across, span(g)]
                    pltpu.make_async_copy(part, part, far_recv.at[w, g]).wait()

        j = lax.rem(x + turn(t), 4)
        tokens = jnp.concatenate(
            [seg_ref[j].reshape(n * MAIN, width), end_ref[j].reshape(n * 2, width)], axis=0
        )
        gate = jnp.dot(tokens, g_buf[...], preferred_element_type=F32)
        up = jnp.dot(tokens, u_buf[...], preferred_element_type=F32)
        hidden = (gate / (1.0 + jnp.exp(-gate)) * up).astype(BF)
        part_ref[j] = jnp.dot(hidden, d_buf[...], preferred_element_type=F32).astype(BF)
        return 0

    lax.fori_loop(0, 4, expert, 0)
    for d in range(2):
        rs_away(d).start()
    spread_relay(0)

    ones = jnp.ones((16, 256), BF)
    row = lax.broadcasted_iota(jnp.int32, (128, 1), 0)
    swap.wait_recv()
    for c in home:
        c.wait()
    acc_ref[...] = jnp.zeros_like(acc_ref)
    max_ref[...] = jnp.full(max_ref.shape, -1e30, F32)

    def queries_of(c):
        h, i = c // 2, c % 2
        both = jnp.concatenate([near_ref[128 * h : 128 * h + 128], far_ref[128 * h : 128 * h + 128]], axis=1)
        return jnp.where((row // 64) == i, both, jnp.zeros_like(both))

    def score(t, c):
        h = c // 2
        k = keys_ref[lax.rem(z + turn(t // 4), 4), lax.rem(y + turn(t % 4), 4), :, 128 * h : 128 * h + 128]
        return jnp.dot(k, queries_of(c), preferred_element_type=F32)

    def finish(t, c, s):
        h = c // 2
        zz, yy = lax.rem(z + turn(t // 4), 4), lax.rem(y + turn(t % 4), 4)
        before = max_ref[c]
        top = jnp.maximum(before, jnp.max(s, axis=0, keepdims=True))
        p = jnp.exp2((s - top[:1]) * LOG2E).astype(BF)
        add = 0.0
        for k in range(2):
            lo = 256 * k + 128 * h
            vt = jnp.concatenate([values_ref[yy, zz, lo : lo + 128, :], ones], axis=0)
            add = add + jnp.dot(vt, p[256 * k : 256 * k + 256], preferred_element_type=F32)
        acc_ref[c] = acc_ref[c] * jnp.exp2((before - top) * LOG2E)[:1] + add
        max_ref[c] = top

    def rest(w, r):
        two_came(w, r, 1 - via(r)).wait()

    def reach(w, r):
        arrival(two_slot(w, r, 2), twof_recv.at[w, r]).wait()

    pieces = ((rep_ref, got_ref), (tip_ref, last_ref))

    def answer():
        rs_landed()
        low, high = rs_total(0), rs_total(1)
        rep_ref[...] = jnp.concatenate([low, high[: n * MAIN - rows // 2]], axis=0).reshape(n, MAIN, width)
        tip_ref[...] = high[n * MAIN - rows // 2 :].reshape(n, 2, width)
        got_ref[0] = rep_ref[0]
        last_ref[0] = tip_ref[0]

        def put(k, _):
            for w, (src, dst) in enumerate(pieces):
                pltpu.make_async_remote_copy(
                    src_ref=src.at[k], dst_ref=dst.at[k], send_sem=rep_send.at[w], recv_sem=rep_recv.at[w],
                    device_id=(e ^ k, x), device_id_type=MESH,
                ).start()
            return 0

        lax.fori_loop(1, n, put, 0)

    events = {
        0: lambda: rest(1, 0),
        1: lambda: spread_relay(1),
        2: lambda: reach(1, 0),
        3: lambda: (rest(0, 0), spread_relay(3)),
        4: lambda: (rest(0, 1), rest(1, 1)),
        5: lambda: (spread_relay(2), rs_join(0), rs_join(1)),
        6: lambda: reach(1, 1),
        9: lambda: (rest(0, 3), rest(1, 3)),
        10: lambda: (rest(0, 2), reach(1, 3)),
        11: lambda: reach(0, 0),
        12: lambda: (reach(0, 1), answer()),
        13: lambda: (reach(0, 3), rest(1, 2)),
        14: lambda: (reach(0, 2), reach(1, 2)),
    }
    s_ref[0] = score(0, 0)

    def attend_block(t, _):
        for k, act in events.items():
            @pl.when(t == k)
            def _(act=act):
                act()
        for c in range(4):
            s_ref[(c + 1) % 2] = score(t, c + 1) if c < 3 else score(jnp.minimum(t + 1, 15), 0)
            finish(t, c, s_ref[c % 2])
        return 0

    lax.fori_loop(0, 16, attend_block, 0)

    mid = acc_ref.shape[2] // 2
    acc_ref[:, 136:144, :] = max_ref[...]
    trade = pltpu.make_async_remote_copy(
        src_ref=acc_ref.at[:, :, pl.ds(mid, mid)], dst_ref=swap_ref, send_sem=out_sem.at[0], recv_sem=out_sem.at[1],
        device_id=(e ^ 1, x), device_id_type=MESH,
    )
    trade.start()
    trade.wait_recv()
    heads = []
    for h in range(2):
        maps = []
        for i in range(2):
            c = 2 * h + i
            a_max, b_max = acc_ref[c, 136:137, :mid], swap_ref[c, 136:137, :]
            top = jnp.maximum(a_max, b_max)
            fa, fb = jnp.exp2((a_max - top) * LOG2E), jnp.exp2((b_max - top) * LOG2E)
            totals = acc_ref[c, 128:129, :mid] * fa + swap_ref[c, 128:129, :] * fb
            maps.append((acc_ref[c, :128, :mid] * fa + swap_ref[c, :128, :] * fb) / totals)
        head = maps[0] - lam_ref[h : h + 1, :] * maps[1]
        mean = jnp.mean(head * head, axis=0, keepdims=True)
        heads.append((head * lax.rsqrt(mean + epsilon) * gain_ref[...] * (1.0 - init_lambda)).astype(BF))
    attended = jnp.concatenate(heads, axis=0).astype(F32).T.astype(BF)
    tokens = mp_ref.shape[1]
    for j in range(4):
        mp_ref[j] = jnp.dot(
            attended[j * tokens : j * tokens + tokens], w_buf[...], preferred_element_type=F32
        ).astype(BF)
    mx_away, mx_plain, mx_join, mx_total, mx_landed, mx_done = scatter(
        mp_ref, tokens // 2, ma_ref, ml_ref, ms_ref, mix_send, mix_recv
    )
    for d in range(2):
        mx_away(d).start()
    for d in range(2):
        mx_plain(d).start()
    for d in range(2):
        mx_join(d)
    for w, (src, dst) in enumerate(pieces):
        moved = dst.at[pl.ds(1, n - 1)]
        pltpu.make_async_copy(moved, moved, rep_recv.at[w]).wait()
        pltpu.make_async_copy(moved, moved, rep_send.at[w]).wait()
    mx_landed()
    mixer_ref[...] = jnp.concatenate([mx_total(0), mx_total(1)], axis=0)

    mx_done()
    rs_done()
    trade.wait_send()
    swap.wait_send()
    for w, (src, dst) in enumerate(pairs):
        sent = dst.at[x, pl.ds(1, n - 1)]
        pltpu.make_async_copy(sent, sent, put_send.at[w]).wait()
        for g in range(GROUPS):
            for d in range(2):
                near(w, g, d).wait_send()
            far(w, g).wait_send()
        for r in range(4):
            two_far(w, r).wait_send()
            for d in range(2):
                two_near(w, r, d).wait_send()
        for g in range(2):
            one_far(w, g).wait_send()
            for d in range(2):
                one_near(w, g, d).wait_send()


def turn(t):
    return t + (t // 2) * (1 - 2 * (t % 2))


def whole(main, tail, gate, up, down, key, value, mine, out_weight, lam, gain):
    n, _, width = main.shape
    dma = pltpu.SemaphoreType.DMA
    hbm, vmem = pl.BlockSpec(memory_space=pl.ANY), pl.BlockSpec(memory_space=pltpu.VMEM)
    rows = n * (MAIN + 2)
    local = mine.shape[1]

    def bf(*shape):
        return pltpu.VMEM(shape, BF)

    def fl(*shape):
        return pltpu.VMEM(shape, F32)

    return pl.pallas_call(
        whole_kernel,
        out_shape=(
            jax.ShapeDtypeStruct((local // 4, width), BF),
            jax.ShapeDtypeStruct(main.shape, BF),
            jax.ShapeDtypeStruct(tail.shape, BF),
        ),
        in_specs=[hbm] * 9 + [vmem] * 2,
        out_specs=(vmem,) * 3,
        scratch_shapes=[
            bf(4, n, MAIN, width), bf(4, n, 2, width), bf(*gate.shape), bf(*up.shape), bf(*down.shape),
            bf(4, rows, width), bf(4, 4, *key.shape), bf(4, 4, *value.shape), bf(*mine.shape), bf(*mine.shape),
            bf(*out_weight.shape),
            bf(2, rows // 2, width), bf(2, 2, rows // 2, width), bf(2, rows // 2, width),
            bf(n, MAIN, width), bf(n, 2, width),
            fl(4, 144, 2 * local), fl(4, 8, 2 * local), fl(2, 512, 2 * local), fl(4, 144, local),
            bf(4, local // 4, width), bf(2, local // 8, width), bf(2, 2, local // 8, width), bf(2, local // 8, width),
            dma((2,)), dma((5,)), dma((2,)), dma((2, GROUPS)), dma((2, 2, GROUPS)), dma((2, 2, GROUPS)),
            dma((2, GROUPS)), dma((2, GROUPS)),
            dma((2,)), dma((2,)), dma((2, 2, 2)), dma((2, 2, 2)), dma((2, 2)), dma((2, 2)),
            dma((2, 2, 4)), dma((2, 2, 4)), dma((2, 4)), dma((2, 4)),
            dma((3, 2)), dma((3, 2)), dma((3, 2)), dma((3, 2)), dma((2,)), dma((2,)), dma((2,)),
        ],
        compiler_params=pltpu.CompilerParams(
            collective_id=0, has_side_effects=True, vmem_limit_bytes=VM
        ),
        name="layer",
    )(main, tail, gate, up, down, key, value, mine, out_weight, lam, gain)


def per_device(
    queries, key_rows, value_rows, lambdas, head_gain, out_weight, moe_input, moe_gain,
    routes, route_logits, expert_gate, expert_up, expert_down,
):
    width = out_weight.shape[1]
    token_count, top_count = routes.shape
    n = lax.axis_size("ep")
    moe_float = moe_input.astype(F32)
    normed = (
        moe_float
        * lax.rsqrt(jnp.mean(moe_float * moe_float, axis=-1, keepdims=True) + epsilon)
        * moe_gain
    ).astype(BF)
    gate_weights = jax.nn.softmax(route_logits, axis=-1)
    flat_routes = routes.reshape(-1)
    chosen = (flat_routes[:, None] == jnp.arange(n, dtype=jnp.int32)[None, :]).astype(jnp.int32)
    rank = jnp.sum((jnp.cumsum(chosen, axis=0) - chosen) * chosen, axis=1)
    step = flat_routes ^ lax.axis_index("ep")
    place = jnp.where(rank < MAIN, step * MAIN + rank, n * MAIN + step * 2 + rank - MAIN)
    place = place.reshape(token_count, top_count)
    slots = jnp.arange(n * (MAIN + 2), dtype=jnp.int32)
    dispatch = jnp.any(place[None, :, :] == slots[:, None, None], axis=-1).astype(BF)
    outgoing = jnp.dot(dispatch, normed, preferred_element_type=F32).astype(BF)
    mine = (queries * jnp.asarray(0.125, BF)).T
    values_t = value_rows.T
    value = jnp.concatenate([values_t[:, :256], values_t[:, 256:]], axis=0)
    lam = jnp.broadcast_to(lambdas[:, None], (2, queries.shape[0]))
    mixer_out, got, got_end = whole(
        outgoing[: n * MAIN].reshape(n, MAIN, width), outgoing[n * MAIN :].reshape(n, 2, width),
        expert_gate[0], expert_up[0], expert_down[0], key_rows, value, mine, out_weight, lam, head_gain[:, None],
    )
    weights = jnp.sum(
        jnp.where(place[:, :, None] == slots, gate_weights[:, :, None], 0.0), axis=1
    )
    high = weights.astype(BF)
    low = (weights - high.astype(F32)).astype(BF)
    both = jnp.concatenate([got.reshape(n * MAIN, width), got_end.reshape(n * 2, width)], axis=0)
    expert_out = (
        jnp.dot(high, both, preferred_element_type=F32) + jnp.dot(low, both, preferred_element_type=F32)
    ).astype(BF)
    return (mixer_out, expert_out)


def solution(mesh):
    placed = (
        P("ep", "tp"),
        P("ep", "tp"),
        P("ep", "tp"),
        P("tp"),
        P(),
        P("tp", None),
        P(("ep", "tp"), None),
        P(),
        P(("ep", "tp"), None),
        P(("ep", "tp"), None),
        P("ep", None, "tp"),
        P("ep", None, "tp"),
        P("ep", "tp", None),
    )
    return jax.shard_map(
        per_device,
        mesh=mesh,
        in_specs=placed,
        out_specs=(P(("ep", "tp"), None), P(("ep", "tp"), None)),
        check_vma=False,
    )
```
